32 devices in a mesh: kv: 8 (over z, x), tp: 4 (over y, core).
Axes of the slice: x: 2, y: 2, z: 4, core: 2. Of those that a mesh axis runs over, the one named last changes fastest.
Arguments:
- tokens: bfloat16 [384, 2048], P(None, 'kv'), may hold values from -40 to 40
- norm_gain: float32 [2048], P('kv'), may hold values from 0.1 to 1.9
- w_query: bfloat16 [2048, 1024], P('kv', 'tp'), may hold values from -0.088388348 to 0.088388348
- w_key: bfloat16 [2048, 1024], P('kv', 'tp'), may hold values from -0.125 to 0.125
- w_value: bfloat16 [2048, 1024], P('kv', 'tp'), may hold values from -0.125 to 0.125
- w_gate: bfloat16 [2048, 16], replicated, may hold values from -0.125 to 0.125
- gate_bias: float32 [16], replicated, may hold values from -1 to 3
- w_out: bfloat16 [1024, 2048], P('tp', 'kv'), may hold values from -0.1875 to 0.1875
- keys_cache: bfloat16 [24, 4096, 1024], P(None, 'kv', 'tp'), may hold values from -512 to 512
- values_cache: bfloat16 [24, 4096, 1024], P(None, 'kv', 'tp'), may hold values from -6 to 6
- cum_gates: float32 [24, 16, 4096], P(None, 'tp', 'kv'), may hold values from -4496 to 0, as said below
- prior_len: int32 [24], replicated, may hold values from 2048 to 4074, as said below
- accepted: int32 [24], replicated, may hold values from 0 to 6
- parents: int32 [24, 16], replicated, may hold values from -1 to 14, as said below
Outputs:
- mixed_rows: bfloat16 [384, 2048], P('tp', 'kv')
- keys_out: bfloat16 [24, 4096, 1024], P(None, 'kv', 'tp')
- values_out: bfloat16 [24, 4096, 1024], P(None, 'kv', 'tp')
The draws below stay inside these ranges and needn't reach their ends.
Inputs may be any that keep to these rules, and one draw needn't show every extreme that they name: parents[b, 0] = -1 and 0 <= parents[b, j] < j for later j. prior_len is at least half of 4096, and prior_len + accepted + 16 <= 4096. `cum_gates`: non-increasing along positions.
All inputs are finite; a program needn't handle non-finite values.
Results may differ from the reference program's by a relative error of at most 0.04.
Values may be sent and summed in bfloat16 or wider, within the bound.
A program may use at most 64 MiB of HBM per device.

```python
import jax
import jax.numpy as jnp
from jax import lax

D = 2048
H = 16
HEAD = 64
PROPS = 16
MOST_ACCEPTED = 6
SEQUENCE_TOTAL = 24
LEN_DEV = 512
CACHE_POSITIONS = 4096
ROWS = 384
N_KV = 8
N_TP = 4


def token_floats(token_key):
    random_keys = jax.random.split(token_key, 3)
    normal_part = jax.random.normal(random_keys[0], (ROWS, D), jnp.float32)
    row_scale = jnp.exp(jax.random.uniform(random_keys[1], (ROWS, 1), jnp.float32, jnp.log(0.3), jnp.log(3.0)))
    column_rise = jnp.exp(jnp.log(3.0) * jnp.arange(D, dtype=jnp.float32)[None, :] / D)
    column_spread = jnp.exp(jax.random.uniform(random_keys[2], (1, D), jnp.float32, jnp.log(0.5), jnp.log(2.0)))
    return jnp.clip(normal_part * row_scale * column_rise * column_spread, -40.0, 40.0)


def query_floats(weight_key):
    drawn = jax.random.truncated_normal(weight_key, -4.0, 4.0, (D, H * HEAD), jnp.float32)
    return drawn * D ** (-0.5)


def draw_tokens(key, part):
    return token_floats(jax.random.fold_in(key, 101)).astype(jnp.bfloat16)


def draw_w_query(key, part):
    return query_floats(jax.random.fold_in(key, 202)).astype(jnp.bfloat16)


def draw_keys_cache(key, part):
    random_keys = jax.random.split(jax.random.fold_in(key, 303), 1)
    result = jax.random.normal(random_keys[0], (SEQUENCE_TOTAL, CACHE_POSITIONS, H * HEAD), jnp.float32)
    result = jnp.clip(result, -6.0, 6.0)
    return jnp.clip(result, -512.0, 512.0).astype(jnp.bfloat16)


def draw_cum_gates(key, part):
    random_keys = jax.random.split(key, 8)
    ranking = jax.random.permutation(random_keys[0], H)
    quick_count = H // 2
    fast_decay_heads = (ranking < quick_count)[None, :, None]
    quick_rate = jnp.exp(jax.random.uniform(random_keys[1], (SEQUENCE_TOTAL, H, 1), jnp.float32, jnp.log(1.0 / 100.0), jnp.log(1.0 / 30.0)))
    slow_rate = jnp.exp(jax.random.uniform(random_keys[2], (SEQUENCE_TOTAL, H, 1), jnp.float32, jnp.log(0.1), jnp.log(0.4))) / CACHE_POSITIONS
    decay_rates = jnp.where(fast_decay_heads, quick_rate, slow_rate)
    block_count = CACHE_POSITIONS // LEN_DEV
    block_multiplier = jnp.exp(jax.random.uniform(random_keys[3], (SEQUENCE_TOTAL, 1, block_count, 1), jnp.float32, 0.0, jnp.log(4.0)))
    block_multiplier = jnp.broadcast_to(block_multiplier, (SEQUENCE_TOTAL, 1, block_count, LEN_DEV)).reshape(SEQUENCE_TOTAL, 1, CACHE_POSITIONS)
    jitter_level = jax.random.uniform(random_keys[4], (SEQUENCE_TOTAL, H, CACHE_POSITIONS), jnp.float32, 0.4, 1.6)
    spike_position = jax.random.randint(random_keys[5], (SEQUENCE_TOTAL, 1, CACHE_POSITIONS), 0, CACHE_POSITIONS) < 2
    dropped_fraction = jax.random.uniform(random_keys[6], (SEQUENCE_TOTAL, H, CACHE_POSITIONS), jnp.float32, 0.2, 0.5)
    spike_events = jnp.where(spike_position & jnp.logical_not(fast_decay_heads), jnp.log(1.0 - dropped_fraction), 0.0)
    gate_increments = spike_events - decay_rates * block_multiplier * jitter_level
    head_offset = jax.random.uniform(random_keys[7], (SEQUENCE_TOTAL, H, 1), jnp.float32, 0.0, 320.0)
    return (jnp.cumsum(gate_increments, axis=2) - head_offset).astype(jnp.float32)


def draw_prior_len(key, part):
    return jax.random.randint(key, (SEQUENCE_TOTAL,), CACHE_POSITIONS // 2, CACHE_POSITIONS - PROPS - MOST_ACCEPTED + 1, dtype=jnp.int32)


def draw_parents(key, part):
    columns = jnp.arange(PROPS, dtype=jnp.int32)
    random_bits = jax.random.randint(key, (SEQUENCE_TOTAL, PROPS), 0, 1 << 20, dtype=jnp.int32)
    picked = random_bits % jnp.maximum(columns, 1)[None, :]
    return jnp.where(columns[None, :] == 0, -1, picked).astype(jnp.int32)


def set_ends(values, own_key, smallest, largest):
    place = [jax.random.randint(jax.random.fold_in(own_key, axis), (), 0, length) for axis, length in enumerate(values.shape)]
    longest = values.shape.index(max(values.shape))
    next_to = place[:longest] + [(place[longest] + 1) % values.shape[longest]] + place[longest + 1:]
    return values.at[tuple(place)].set(smallest).at[tuple(next_to)].set(largest)


def steps_of(key, shape, pieces, least, high):
    loudness = 1.0
    for axis_at, parts in pieces:
        heights = jax.random.uniform(jax.random.fold_in(jax.random.fold_in(key, 6), axis_at), (parts,), jnp.float32, least / len(pieces), high / len(pieces))
        loudness = loudness * jnp.repeat(jnp.exp(heights), shape[axis_at] // parts).reshape((-1,) + (1,) * (len(shape) - 1 - axis_at))
    return loudness


def centred(stream_key, extent, spread, limit, cuts=(), held_as=jnp.bfloat16):
    values = jax.random.normal(stream_key, extent, jnp.float32) * spread
    if len(cuts) > 0:
        values = steps_of(stream_key, extent, cuts, -0.22, 0.18) * values
    return jnp.clip(values, min=-limit, max=limit).astype(held_as)


def setup_inputs(seed: int = 0) -> dict:
    streams_of = jax.random.split(jax.random.key(seed), 15)
    tokens = draw_tokens(jax.random.fold_in(streams_of[14], 71), 0)
    norm_gain = jnp.clip(1.0 + 0.18 * jax.random.normal(streams_of[1], (D,), jnp.float32), 0.1, 1.9)
    w_query = draw_w_query(jax.random.fold_in(streams_of[14], 71), 0)
    w_key = centred(streams_of[3], (D, H * HEAD), D ** -0.5, 0.125, ((0, 8), (1, 4)))
    w_value = centred(streams_of[4], (D, H * HEAD), D ** -0.5, 0.125, ((0, 8), (1, 4)))
    w_gate = centred(streams_of[5], (D, H), D ** -0.5, 0.125)
    gate_bias = jnp.clip(jax.random.uniform(streams_of[6], (H,), jnp.float32, -1.0, 3.0), -1.0, 3.0)
    w_out = centred(streams_of[7], (H * HEAD, D), (H * HEAD) ** -0.5, 0.1875, ((0, 4), (1, 8)))
    keys_cache = draw_keys_cache(jax.random.fold_in(streams_of[14], 71), 0)
    values_cache = centred(streams_of[9], (SEQUENCE_TOTAL, CACHE_POSITIONS, H * HEAD), 1.0, 6.0, ((1, 8), (2, 4)))
    cum_gates = draw_cum_gates(jax.random.fold_in(streams_of[14], 71), 0)
    prior_len = draw_prior_len(jax.random.fold_in(streams_of[14], 71), 0)
    accepted = set_ends(jax.random.randint(streams_of[12], (SEQUENCE_TOTAL,), 0, MOST_ACCEPTED + 1), jax.random.fold_in(streams_of[12], 1), 0, MOST_ACCEPTED).astype(jnp.int32)
    parents = draw_parents(jax.random.fold_in(streams_of[14], 71), 0)
    return {"tokens": tokens, "norm_gain": norm_gain, "w_query": w_query, "w_key": w_key, "w_value": w_value, "w_gate": w_gate, "gate_bias": gate_bias, "w_out": w_out, "keys_cache": keys_cache, "values_cache": values_cache, "cum_gates": cum_gates, "prior_len": prior_len, "accepted": accepted, "parents": parents}


masked_score = -1e+30
norm_eps = 1e-06

def ancestry(parents):
    columns = jnp.arange(PROPS, dtype=jnp.int32)
    parent_link = (parents[:, :, None] == columns[None, None, :]).astype(jnp.float32)
    reached = jnp.eye(PROPS, dtype=jnp.float32)[None] + parent_link
    for squaring in range(PROPS.bit_length()):
        reached = jnp.minimum(jnp.einsum('bij,bjk->bik', reached, reached, precision=lax.Precision.HIGHEST), 1.0)
    return reached

def reference(tokens, norm_gain, w_query, w_key, w_value, w_gate, gate_bias, w_out, keys_cache, values_cache, cum_gates, prior_len, accepted, parents):
    floats = tokens.astype(jnp.float32)
    inv_rms = lax.rsqrt(lax.optimization_barrier(jnp.sum(floats * floats, axis=1)) / D + norm_eps)
    scaled = (floats * norm_gain).astype(jnp.bfloat16)

    def project(weight):
        return inv_rms[:, None] * jnp.dot(scaled, weight, preferred_element_type=jnp.float32)
    queries = project(w_query).astype(jnp.bfloat16)
    new_keys = project(w_key).astype(jnp.bfloat16)
    new_values = project(w_value).astype(jnp.bfloat16)
    log_gates = jax.nn.log_sigmoid(project(w_gate) + gate_bias).reshape(SEQUENCE_TOTAL, PROPS, H)
    reached = ancestry(parents)
    tree_gates = jnp.einsum('bij,bjh->bih', reached, log_gates, precision=lax.Precision.HIGHEST)
    filled = prior_len + accepted
    last_pos = filled - 1
    index_last = jnp.broadcast_to(last_pos[:, None, None], (SEQUENCE_TOTAL, H, 1))
    last_gate = jnp.take_along_axis(cum_gates, index_last, axis=2)[:, :, 0]
    prop_cum = last_gate[:, None, :] + tree_gates
    owners = (last_pos // LEN_DEV).astype(jnp.int32)
    scale = HEAD ** (-0.5)

    def attend(packed):
        seq_query, seq_keys, seq_values, seq_cum, seq_newk, seq_newv, seq_prop, seq_reach, seq_fill, seq_owner = packed
        query_f = seq_query.reshape(PROPS, H, HEAD).astype(jnp.float32)
        keys_f = seq_keys.reshape(CACHE_POSITIONS, H, HEAD).astype(jnp.float32)
        scores = jnp.einsum('ihd,phd->hip', query_f, keys_f) * scale - seq_cum[:, None, :]
        positions = jnp.arange(CACHE_POSITIONS, dtype=jnp.int32)
        valid_keys = positions < seq_fill
        scores = jnp.where(valid_keys[None, None, :], scores, masked_score)
        blocked = scores.reshape(H, PROPS, N_KV, LEN_DEV)
        newk_f = seq_newk.reshape(PROPS, H, HEAD).astype(jnp.float32)
        tree_scores = jnp.einsum('ihd,jhd->hij', query_f, newk_f) * scale - jnp.transpose(seq_prop)[:, None, :]
        tree_live = (seq_reach > 0.5)[None]
        tree_scores = jnp.where(tree_live, tree_scores, masked_score)
        is_owner = jnp.arange(N_KV, dtype=jnp.int32) == seq_owner
        block_max = lax.optimization_barrier(jnp.max(blocked, axis=3))
        tree_max = lax.optimization_barrier(jnp.max(tree_scores, axis=2))
        block_max = jnp.where(is_owner[None, None, :], jnp.maximum(block_max, tree_max[:, :, None]), block_max)
        owner_max = lax.optimization_barrier(jnp.max(jnp.where(is_owner[None, None, :], block_max, masked_score), axis=2))
        valid_blocks = valid_keys.reshape(N_KV, LEN_DEV)[None, None]
        weights = jnp.where(valid_blocks, jnp.exp(blocked - block_max[..., None]), 0.0)
        tree_weights = jnp.where(tree_live, jnp.exp(tree_scores - owner_max[:, :, None]), 0.0)
        block_sums = lax.optimization_barrier(jnp.sum(weights, axis=3)) + jnp.where(is_owner[None, None, :], lax.optimization_barrier(jnp.sum(tree_weights, axis=2))[:, :, None], 0.0)
        values_f = seq_values.reshape(N_KV, LEN_DEV, H, HEAD).astype(jnp.float32)
        newv_f = seq_newv.reshape(PROPS, H, HEAD).astype(jnp.float32)
        rounded = lax.optimization_barrier(weights.astype(jnp.bfloat16)).astype(jnp.float32)
        tree_rounded = lax.optimization_barrier(tree_weights.astype(jnp.bfloat16)).astype(jnp.float32)
        block_values = jnp.einsum('hinp,nphd->hind', rounded, values_f)
        tree_values = jnp.einsum('hij,jhd->hid', tree_rounded, newv_f)
        block_values = block_values + jnp.where(is_owner[None, None, :, None], tree_values[:, :, None, :], 0.0)
        block_values = lax.optimization_barrier(block_values.astype(jnp.bfloat16)).astype(jnp.float32)
        top_score = lax.optimization_barrier(jnp.max(block_max, axis=2))
        rescale = jnp.exp(block_max - top_score[..., None])
        grand_total = lax.optimization_barrier(jnp.sum(rescale * block_sums, axis=2))
        result = lax.optimization_barrier(jnp.sum(rescale[..., None] * block_values, axis=2)) / grand_total[..., None]
        return jnp.transpose(result, (1, 0, 2)).astype(jnp.bfloat16)
    packed = (queries.reshape(SEQUENCE_TOTAL, PROPS, H * HEAD), keys_cache, values_cache, cum_gates, new_keys.reshape(SEQUENCE_TOTAL, PROPS, H * HEAD), new_values.reshape(SEQUENCE_TOTAL, PROPS, H * HEAD), prop_cum, reached, filled, owners)
    attended = lax.map(attend, packed).reshape(ROWS, H * HEAD)
    group = H // N_TP * HEAD
    parted = attended.reshape(ROWS, N_TP, group).astype(jnp.float32)
    weight_groups = w_out.reshape(N_TP, group, D).astype(jnp.float32)
    head_parts = jnp.einsum('rgc,gcd->grd', parted, weight_groups)
    head_parts = lax.optimization_barrier(head_parts.astype(jnp.bfloat16)).astype(jnp.float32)
    mixed_rows = lax.optimization_barrier(jnp.sum(head_parts, axis=0)).astype(jnp.bfloat16)

    def write(cache, new_rows, start):
        return lax.dynamic_update_slice(cache, new_rows, (start.astype(jnp.int32), jnp.zeros((), jnp.int32)))
    keys_out = jax.vmap(write)(keys_cache, new_keys.reshape(SEQUENCE_TOTAL, PROPS, H * HEAD), filled)
    values_out = jax.vmap(write)(values_cache, new_values.reshape(SEQUENCE_TOTAL, PROPS, H * HEAD), filled)
    return (mixed_rows, keys_out, values_out)
```

```python
import functools

import jax
import jax.numpy as jnp
from jax import lax
from jax.experimental import pallas as pl
from jax.experimental.pallas import tpu as pltpu
from jax.sharding import PartitionSpec as P

HEAD = 64
PROPS = 16
LANES = 128
SQUARE_LANE = 96
masked_score = -1e30
norm_eps = 1e-06
MESH = pl.DeviceIdType.MESH
HIGHEST = lax.Precision.HIGHEST
f32, bf16, i32 = jnp.float32, jnp.bfloat16, jnp.int32


def iota(shape, axis):
    return lax.broadcasted_iota(i32, shape, axis)


def split3(x):
    hi = x.astype(bf16).astype(f32)
    mid = (x - hi).astype(bf16).astype(f32)
    return hi, mid, x - hi - mid


def contract_last(a, b, precision=None):
    return lax.dot_general(
        a, b, (((1,), (1,)), ((), ())), preferred_element_type=f32, precision=precision
    )


def project_kernel(
    n_kv,
    heads,
    tokens_ref,
    gain_ref,
    wq_ref,
    wk_ref,
    wv_ref,
    wg_ref,
    bias_ref,
    out_ref,
    part,
    arrived,
    gathered,
    mine,
    send_a,
    recv_a,
    send_b,
    recv_b,
):
    me = lax.axis_index("kv")
    tp = lax.axis_index("tp")
    chunk_rows, depth = tokens_ref.shape[1:]
    width = heads * HEAD
    barrier = pltpu.get_barrier_semaphore()
    for d in range(1, n_kv):
        pl.semaphore_signal(
            barrier, inc=1, device_id={"kv": lax.rem(me + d, n_kv)}, device_id_type=MESH
        )

    total_heads = wg_ref.shape[1]
    lane = iota((total_heads, LANES), 1)
    pick = (iota((total_heads, LANES), 0) == tp * heads + lane % 32) & (lane % 32 < heads) & (lane < 96)
    pick = jnp.where(pick, 1.0, 0.0)
    gate_w = wg_ref[pl.ds(pl.multiple_of(me * depth, depth), depth), :]
    gate_w = jnp.dot(gate_w, pick.astype(bf16), preferred_element_type=f32).astype(bf16)

    def partial_sums(floats):
        scaled = (floats * gain_ref[...]).astype(bf16)
        square = jnp.sum(floats * floats, axis=1, keepdims=True)
        gates = jnp.dot(scaled, gate_w, preferred_element_type=f32)
        gates = jnp.where(iota(gates.shape, 1) == SQUARE_LANE, square, gates)
        products = [
            jnp.dot(scaled, w[...], preferred_element_type=f32).astype(bf16)
            for w in (wq_ref, wk_ref, wv_ref)
        ]
        return products + [gates.astype(bf16)]

    edges = [0, width, 2 * width, 3 * width, 3 * width + LANES]
    if chunk_rows % 16 == 0:
        floats = tokens_ref[...].reshape(n_kv * chunk_rows, depth).astype(f32)
        for piece, low, high in zip(partial_sums(floats), edges[:-1], edges[1:]):
            part[:, :, low:high] = piece.reshape(n_kv, chunk_rows, high - low)
    else:

        def one(c, carry):
            for piece, low, high in zip(
                partial_sums(tokens_ref[c].astype(f32)), edges[:-1], edges[1:]
            ):
                part[c, :, low:high] = piece
            return carry

        lax.fori_loop(0, n_kv, one, 0)

    pl.semaphore_wait(barrier, n_kv - 1)
    copies = []
    for d in range(1, n_kv):
        peer = lax.rem(me + d, n_kv)
        copy = pltpu.make_async_remote_copy(
            src_ref=part.at[peer],
            dst_ref=arrived.at[d - 1],
            send_sem=send_a.at[d - 1],
            recv_sem=recv_a.at[d - 1],
            device_id={"kv": peer},
            device_id_type=MESH,
        )
        copy.start()
        copies.append(copy)
    total = part[me].astype(f32)
    for d in range(1, n_kv):
        copies[d - 1].wait_recv()
        total = total + arrived[d - 1].astype(f32)
    tail = total[:, 3 * width :]
    tail_lane = iota(tail.shape, 1)
    square = jnp.sum(jnp.where(tail_lane == SQUARE_LANE, tail, 0.0), axis=1, keepdims=True)
    inv_rms = lax.rsqrt(square / (n_kv * depth) + norm_eps)
    bias = jnp.dot(
        jnp.broadcast_to(bias_ref[...], (8, total_heads)),
        pick,
        preferred_element_type=f32,
        precision=HIGHEST,
    )[0:1]
    pre = inv_rms * tail + bias
    log_gates = jnp.minimum(pre, 0.0) - jnp.log1p(jnp.exp(-jnp.abs(pre)))
    hi, mid, low = split3(log_gates)
    packed = jnp.where(tail_lane < 32, hi, jnp.where(tail_lane < 64, mid, low))
    packed = jnp.where((tail_lane % 32 < heads) & (tail_lane < 96), packed, 0.0)
    mine[:, : 3 * width] = (inv_rms * total[:, : 3 * width]).astype(bf16)
    mine[:, 3 * width :] = packed.astype(bf16)
    back = []
    for d in range(1, n_kv):
        copy = pltpu.make_async_remote_copy(
            src_ref=mine,
            dst_ref=gathered.at[me],
            send_sem=send_b.at[d - 1],
            recv_sem=recv_b.at[d - 1],
            device_id={"kv": lax.rem(me + d, n_kv)},
            device_id_type=MESH,
        )
        copy.start()
        back.append(copy)
    out_ref[me] = mine[...]
    for d in range(1, n_kv):
        source = lax.rem(me + n_kv - d, n_kv)
        back[d - 1].wait_recv()
        out_ref[source] = gathered[source]
    for copy in copies + back:
        copy.wait_send()


def attend_kernel(
    heads, prior_s, accepted_s, proj_ref, parents_ref, k_ref, v_ref, cum_ref, ko_ref, vo_ref, out_ref
):
    group = k_ref.shape[0]
    length = k_ref.shape[1]
    width = heads * HEAD
    rows = group * PROPS
    score_rows = heads * PROPS
    offset = lax.axis_index("kv") * length
    step = pl.program_id(0)

    row = iota((rows, rows), 0)
    column = iota((rows, rows), 1)
    parent = parents_ref[...]
    link = (parent + (row // PROPS) * PROPS == column) & (parent >= 0)
    reached = jnp.where(link | (row == column), 1.0, 0.0)
    for squaring in range((PROPS - 1).bit_length()):
        reached = jnp.minimum(
            jnp.dot(reached.astype(bf16), reached.astype(bf16), preferred_element_type=f32), 1.0
        )
    tree_gates = jnp.dot(
        reached.astype(bf16), proj_ref[:, 3 * width :], preferred_element_type=f32
    )
    lane = iota((score_rows, LANES), 1)
    row_head = iota((score_rows, LANES), 0) // PROPS
    gate_pick = jnp.where((lane % 32 == row_head) & (lane < 96), 1.0, 0.0)
    same_head = iota((score_rows, width), 0) // PROPS == iota((score_rows, width), 1) // HEAD
    position = iota((score_rows, length), 1)
    window = 2 * PROPS
    for b in range(group):
        span = slice(b * PROPS, (b + 1) * PROPS)
        seq = step * group + b
        limit = prior_s[seq] + accepted_s[seq] - offset
        owner = jnp.where((limit >= 1) & (limit <= length), 1.0, 0.0)
        new_k = proj_ref[span, width : 2 * width]
        new_v = proj_ref[span, 2 * width : 3 * width]
        query = jnp.concatenate([proj_ref[span, :width]] * heads, axis=0).astype(f32)
        query = (jnp.where(same_head, query, 0.0) * HEAD ** (-0.5)).astype(bf16)
        cum = jnp.concatenate(
            [
                jnp.broadcast_to(cum_ref[b, h : h + 1, :], (PROPS, length))
                for h in range(heads)
            ],
            axis=0,
        )
        valid = position < limit
        scores = jnp.where(valid, contract_last(query, k_ref[b]) - cum, masked_score)
        last = jnp.sum(jnp.where(position == limit - 1, cum, 0.0), axis=1, keepdims=True)
        prop_cum = last + contract_last(gate_pick, tree_gates[span], HIGHEST)
        live = jnp.concatenate([reached[span, span]] * heads, axis=0) * owner > 0.5
        tree = jnp.where(live, contract_last(query, new_k) - prop_cum, masked_score)
        top = jnp.maximum(
            jnp.max(scores, axis=1, keepdims=True), jnp.max(tree, axis=1, keepdims=True)
        )
        weights = jnp.where(valid, jnp.exp(scores - top), 0.0)
        tree_weights = jnp.where(live, jnp.exp(tree - top), 0.0)
        total = jnp.sum(weights, axis=1, keepdims=True) + jnp.sum(
            tree_weights, axis=1, keepdims=True
        )
        values = jnp.dot(weights.astype(bf16), v_ref[b], preferred_element_type=f32)
        values = values + jnp.dot(tree_weights.astype(bf16), new_v, preferred_element_type=f32)
        values = jnp.where(same_head, values, 0.0)
        t_hi, t_mid, t_low = split3(top)
        s_hi, s_mid, s_low = split3(total)
        part = lane // 16
        packed = jnp.where(
            part == 0,
            t_hi,
            jnp.where(
                part == 1, t_mid, jnp.where(part == 2, t_low, jnp.where(part == 3, s_hi, s_mid))
            ),
        )
        packed = jnp.where((lane % 16 == row_head) & (part < 5), packed, 0.0)
        picked_values = values[:PROPS]
        picked_packed = packed[:PROPS]
        for h in range(1, heads):
            picked_values = picked_values + values[h * PROPS : (h + 1) * PROPS]
            picked_packed = picked_packed + packed[h * PROPS : (h + 1) * PROPS]
        out_ref[span, :width] = picked_values.astype(bf16)
        out_ref[span, width:] = picked_packed.astype(bf16)

        start = pl.multiple_of(jnp.clip(limit, 0, length - window) // PROPS * PROPS, PROPS)
        select = start + iota((window, PROPS), 0) - limit == iota((window, PROPS), 1)
        select = jnp.where(select, 1.0, 0.0).astype(bf16)
        slot = start + iota((window, width), 0) - limit
        inside = (slot >= 0) & (slot < PROPS)
        for source, target, fresh in ((k_ref, ko_ref, new_k), (v_ref, vo_ref, new_v)):
            target[b] = source[b]
            placed = jnp.dot(select, fresh, preferred_element_type=f32)
            old = source[b, pl.ds(start, window), :].astype(f32)
            target[b, pl.ds(start, window), :] = jnp.where(inside, placed, old).astype(bf16)


def combine_kernel(
    n_kv,
    n_tp,
    heads,
    parts_ref,
    w_ref,
    out_ref,
    arrived,
    mine,
    gathered,
    partial,
    landed,
    send_a,
    recv_a,
    send_b,
    recv_b,
    send_c,
    recv_c,
):
    me = lax.axis_index("kv")
    tp = lax.axis_index("tp")
    width = heads * HEAD
    chunk_rows = parts_ref.shape[1]
    share = n_kv // n_tp
    barrier = pltpu.get_barrier_semaphore()
    for d in range(1, n_kv):
        pl.semaphore_signal(
            barrier, inc=1, device_id={"kv": lax.rem(me + d, n_kv)}, device_id_type=MESH
        )
    for d in range(1, n_tp):
        pl.semaphore_signal(
            barrier, inc=1, device_id={"tp": lax.rem(tp + d, n_tp)}, device_id_type=MESH
        )
    pl.semaphore_wait(barrier, n_kv - 1 + n_tp - 1)
    first = []
    for d in range(1, n_kv):
        peer = lax.rem(me + d, n_kv)
        copy = pltpu.make_async_remote_copy(
            src_ref=parts_ref.at[peer],
            dst_ref=arrived.at[d - 1],
            send_sem=send_a.at[d - 1],
            recv_sem=recv_a.at[d - 1],
            device_id={"kv": peer},
            device_id_type=MESH,
        )
        copy.start()
        first.append(copy)
    lane = iota((LANES, width), 0)
    fits = lane % 16 == iota((LANES, width), 1) // HEAD
    spread_top = jnp.where(fits & (lane < 48), 1.0, 0.0).astype(bf16)
    spread_sum = jnp.where(fits & (lane >= 48) & (lane < 80), 1.0, 0.0).astype(bf16)

    def unpack(block):
        packed = block[:, width:]
        return (
            jnp.dot(packed, spread_top, preferred_element_type=f32),
            jnp.dot(packed, spread_sum, preferred_element_type=f32),
            block[:, :width].astype(f32),
        )

    top, sums, values = unpack(parts_ref[me])
    for d in range(1, n_kv):
        first[d - 1].wait_recv()
        other_top, other_sums, other_values = unpack(arrived[d - 1])
        new_top = jnp.maximum(top, other_top)
        here, there = jnp.exp(top - new_top), jnp.exp(other_top - new_top)
        sums = here * sums + there * other_sums
        values = here * values + there * other_values
        top = new_top
    mine[...] = (values / sums).astype(bf16)
    second = []
    for d in range(1, n_kv):
        copy = pltpu.make_async_remote_copy(
            src_ref=mine,
            dst_ref=gathered.at[me],
            send_sem=send_b.at[d - 1],
            recv_sem=recv_b.at[d - 1],
            device_id={"kv": lax.rem(me + d, n_kv)},
            device_id_type=MESH,
        )
        copy.start()
        second.append(copy)
    gathered[me] = mine[...]
    for copy in second:
        copy.wait_recv()
    if chunk_rows % 16 == 0:
        attended = gathered[...].reshape(n_kv * chunk_rows, width)
        product = jnp.dot(attended, w_ref[...], preferred_element_type=f32).astype(bf16)
        partial[...] = product.reshape(partial.shape)
    else:

        def one(c, carry):
            partial[c] = jnp.dot(gathered[c], w_ref[...], preferred_element_type=f32).astype(bf16)
            return carry

        lax.fori_loop(0, n_kv, one, 0)
    third = []
    for d in range(1, n_tp):
        peer = lax.rem(tp + d, n_tp)
        copy = pltpu.make_async_remote_copy(
            src_ref=partial.at[pl.ds(peer * share, share)],
            dst_ref=landed.at[d - 1],
            send_sem=send_c.at[d - 1],
            recv_sem=recv_c.at[d - 1],
            device_id={"tp": peer},
            device_id_type=MESH,
        )
        copy.start()
        third.append(copy)
    total = partial[pl.ds(tp * share, share)].astype(f32)
    for d in range(1, n_tp):
        third[d - 1].wait_recv()
        total = total + landed[d - 1].astype(f32)
    out_ref[...] = total.astype(bf16)
    for copy in first + second + third:
        copy.wait_send()


def shards(
    n_kv,
    n_tp,
    tokens,
    norm_gain,
    w_query,
    w_key,
    w_value,
    w_gate,
    gate_bias,
    w_out,
    keys_cache,
    values_cache,
    cum_gates,
    prior_len,
    accepted,
    parents,
):
    row_count, depth = tokens.shape
    seq_count, length, width = keys_cache.shape
    heads = width // HEAD
    chunk_rows = row_count // n_kv
    columns = w_out.shape[1]
    vmem = pl.BlockSpec(memory_space=pltpu.VMEM)
    dma = pltpu.SemaphoreType.DMA
    proj_width = 3 * width + LANES
    out_width = width + LANES

    projected = pl.pallas_call(
        functools.partial(project_kernel, n_kv, heads),
        out_shape=jax.ShapeDtypeStruct((n_kv, chunk_rows, proj_width), bf16),
        in_specs=[vmem] * 7,
        out_specs=vmem,
        scratch_shapes=[
            pltpu.VMEM((n_kv, chunk_rows, proj_width), bf16),
            pltpu.VMEM((n_kv - 1, chunk_rows, proj_width), bf16),
            pltpu.VMEM((n_kv, chunk_rows, proj_width), bf16),
            pltpu.VMEM((chunk_rows, proj_width), bf16),
        ]
        + [dma((n_kv - 1,))] * 4,
        compiler_params=pltpu.CompilerParams(collective_id=0, has_side_effects=True),
        name="project",
    )(
        tokens.reshape(n_kv, chunk_rows, depth),
        norm_gain.reshape(1, depth),
        w_query,
        w_key,
        w_value,
        w_gate,
        gate_bias.reshape(1, -1),
    )
    projected = projected.reshape(row_count, proj_width)

    group = next(g for g in (4, 3, 2, 1) if seq_count % g == 0)
    rows = group * PROPS
    cache_spec = pl.BlockSpec((group, length, width), lambda s, *_: (s, 0, 0))
    keys_out, values_out, parts = pl.pallas_call(
        functools.partial(attend_kernel, heads),
        out_shape=(
            jax.ShapeDtypeStruct(keys_cache.shape, bf16),
            jax.ShapeDtypeStruct(values_cache.shape, bf16),
            jax.ShapeDtypeStruct((row_count, out_width), bf16),
        ),
        grid_spec=pltpu.PrefetchScalarGridSpec(
            num_scalar_prefetch=2,
            grid=(seq_count // group,),
            in_specs=[
                pl.BlockSpec((rows, proj_width), lambda s, *_: (s, 0)),
                pl.BlockSpec((rows, 1), lambda s, *_: (s, 0)),
                cache_spec,
                cache_spec,
                pl.BlockSpec((group, heads, length), lambda s, *_: (s, 0, 0)),
            ],
            out_specs=[
                cache_spec,
                cache_spec,
                pl.BlockSpec((rows, out_width), lambda s, *_: (s, 0)),
            ],
        ),
        name="attend",
    )(
        prior_len,
        accepted,
        projected,
        parents.reshape(row_count, 1),
        keys_cache,
        values_cache,
        cum_gates,
    )

    mixed = pl.pallas_call(
        functools.partial(combine_kernel, n_kv, n_tp, heads),
        out_shape=jax.ShapeDtypeStruct((n_kv // n_tp, chunk_rows, columns), bf16),
        in_specs=[vmem] * 2,
        out_specs=vmem,
        scratch_shapes=[
            pltpu.VMEM((n_kv - 1, chunk_rows, out_width), bf16),
            pltpu.VMEM((chunk_rows, width), bf16),
            pltpu.VMEM((n_kv, chunk_rows, width), bf16),
            pltpu.VMEM((n_kv, chunk_rows, columns), bf16),
            pltpu.VMEM((n_tp - 1, n_kv // n_tp, chunk_rows, columns), bf16),
        ]
        + [dma((n_kv - 1,))] * 4
        + [dma((n_tp - 1,))] * 2,
        compiler_params=pltpu.CompilerParams(collective_id=1, has_side_effects=True),
        name="combine",
    )(parts.reshape(n_kv, chunk_rows, out_width), w_out)
    return (mixed.reshape(row_count // n_tp, columns), keys_out, values_out)


def solution(mesh):
    placed = (
        P(None, "kv"),
        P("kv"),
        P("kv", "tp"),
        P("kv", "tp"),
        P("kv", "tp"),
        P(),
        P(),
        P("tp", "kv"),
        P(None, "kv", "tp"),
        P(None, "kv", "tp"),
        P(None, "tp", "kv"),
        P(),
        P(),
        P(),
    )
    return jax.shard_map(
        functools.partial(shards, mesh.shape["kv"], mesh.shape["tp"]),
        mesh=mesh,
        in_specs=placed,
        out_specs=(P("tp", "kv"), P(None, "kv", "tp"), P(None, "kv", "tp")),
        check_vma=False,
    )
```

```python
import functools

import jax
import jax.numpy as jnp
from jax import lax
from jax.experimental import pallas as pl
from jax.experimental.pallas import tpu as pltpu
from jax.sharding import PartitionSpec as P

HEAD = 64
PROPS = 16
LANES = 128
SQUARE_LANE = 96
masked_score = -1e30
norm_eps = 1e-06
MESH = pl.DeviceIdType.MESH
HIGHEST = lax.Precision.HIGHEST
f32, bf16, i32 = jnp.float32, jnp.bfloat16, jnp.int32


def iota(shape, axis):
    return lax.broadcasted_iota(i32, shape, axis)


def split3(x):
    hi = x.astype(bf16).astype(f32)
    mid = (x - hi).astype(bf16).astype(f32)
    return hi, mid, x - hi - mid


def contract_last(a, b, precision=None):
    return lax.dot_general(
        a, b, (((1,), (1,)), ((), ())), preferred_element_type=f32, precision=precision
    )


def project_kernel(
    n_kv,
    heads,
    tokens_ref,
    gain_ref,
    wq_ref,
    wk_ref,
    wv_ref,
    wg_ref,
    bias_ref,
    out_ref,
    part,
    swapped,
    middle,
    arrived,
    gathered,
    mine,
    *sems,
):
    swap_sems, sum_sems, back_sems, last_sems = sems[0:2], sems[2:4], sems[4:6], sems[6:8]
    me = lax.axis_index("kv")
    tp = lax.axis_index("tp")
    chunk_rows, depth = tokens_ref.shape[1:]
    width = heads * HEAD
    barrier = pltpu.get_barrier_semaphore()
    for d in range(1, n_kv):
        pl.semaphore_signal(
            barrier, inc=1, device_id={"kv": lax.rem(me + d, n_kv)}, device_id_type=MESH
        )

    total_heads = bias_ref.shape[1]
    lane = iota((total_heads, LANES), 1)
    pick = (iota((total_heads, LANES), 0) == tp * heads + lane % 32) & (lane % 32 < heads) & (lane < 96)
    pick = jnp.where(pick, 1.0, 0.0)
    if depth % LANES == 0:
        slot = iota((LANES, total_heads), 0)
        pick_rows = iota((LANES, total_heads), 1) == tp * heads + slot % 32
        pick_rows = jnp.where(pick_rows & (slot % 32 < heads) & (slot < 96), 1.0, 0.0)
        gate_w = wg_ref[:, pl.ds(pl.multiple_of(me * depth, depth), depth)]
        gate_w = jnp.dot(pick_rows.astype(bf16), gate_w, preferred_element_type=f32).astype(bf16)
        gate_product = functools.partial(contract_last, b=gate_w)
    else:
        gate_w = wg_ref[pl.ds(pl.multiple_of(me * depth, depth), depth), :]
        gate_w = jnp.dot(gate_w, pick.astype(bf16), preferred_element_type=f32).astype(bf16)
        gate_product = functools.partial(jnp.dot, b=gate_w, preferred_element_type=f32)

    def partial_sums(floats):
        scaled = (floats * gain_ref[...]).astype(bf16)
        square = jnp.sum(floats * floats, axis=1, keepdims=True)
        gates = gate_product(scaled)
        gates = jnp.where(iota(gates.shape, 1) == SQUARE_LANE, square, gates)
        products = [
            jnp.dot(scaled, w[...], preferred_element_type=f32).astype(bf16)
            for w in (wq_ref, wk_ref, wv_ref)
        ]
        return products + [gates.astype(bf16)]

    edges = [0, width, 2 * width, 3 * width, 3 * width + LANES]
    if chunk_rows % 16 == 0:
        floats = tokens_ref[...].reshape(n_kv * chunk_rows, depth).astype(f32)
        for piece, low, high in zip(partial_sums(floats), edges[:-1], edges[1:]):
            blocks = piece.reshape(n_kv, chunk_rows, high - low)
            for c in range(n_kv):
                part[c % 2, c // 2, :, low:high] = blocks[c]
    else:

        def one(c, carry):
            for piece, low, high in zip(
                partial_sums(tokens_ref[c].astype(f32)), edges[:-1], edges[1:]
            ):
                part[lax.rem(c, 2), c // 2, :, low:high] = piece
            return carry

        lax.fori_loop(0, n_kv, one, 0)

    outer = n_kv // 2
    x, z = lax.rem(me, 2), me // 2
    partner = me + 1 - 2 * x
    pieces = [pl.ds(2 * width, width + LANES), pl.ds(0, width), pl.ds(width, width)]

    def send(source, target, sems, at, device):
        copy = pltpu.make_async_remote_copy(
            src_ref=source,
            dst_ref=target,
            send_sem=sems[0].at[at],
            recv_sem=sems[1].at[at],
            device_id={"kv": device},
            device_id_type=MESH,
        )
        copy.start()
        return copy

    pl.semaphore_wait(barrier, n_kv - 1)
    swaps = [
        send(part.at[1 - x, :, :, at], swapped.at[:, :, at], swap_sems, p, partner)
        for p, at in enumerate(pieces)
    ]
    sums = []
    for p, at in enumerate(pieces):
        swaps[p].wait_recv()
        half = part[x, :, :, at].astype(f32) + swapped[:, :, at].astype(f32)
        middle[:, :, at] = half.astype(bf16)
        row = []
        for d in range(1, outer):
            other = lax.rem(z + d, outer)
            row.append(
                send(
                    middle.at[other, :, at],
                    arrived.at[d - 1, :, at],
                    sum_sems,
                    p * (outer - 1) + d - 1,
                    other * 2 + x,
                )
            )
        sums.append(row)
    bias = jnp.dot(
        jnp.broadcast_to(bias_ref[...], (8, total_heads)),
        pick,
        preferred_element_type=f32,
        precision=HIGHEST,
    )[0:1]
    inv_rms = None
    backs = []
    for p, at in enumerate(pieces):
        total = middle[z, :, at].astype(f32)
        for d in range(1, outer):
            sums[p][d - 1].wait_recv()
            total = total + arrived[d - 1, :, at].astype(f32)
        if p == 0:
            tail = total[:, width:]
            tail_lane = iota(tail.shape, 1)
            square = jnp.sum(jnp.where(tail_lane == SQUARE_LANE, tail, 0.0), axis=1, keepdims=True)
            inv_rms = lax.rsqrt(square / (n_kv * depth) + norm_eps)
            pre = inv_rms * tail + bias
            log_gates = jnp.minimum(pre, 0.0) - jnp.log1p(jnp.exp(-jnp.abs(pre)))
            hi, mid, low = split3(log_gates)
            packed = jnp.where(tail_lane < 32, hi, jnp.where(tail_lane < 64, mid, low))
            packed = jnp.where((tail_lane % 32 < heads) & (tail_lane < 96), packed, 0.0)
            mine[:, 3 * width :] = packed.astype(bf16)
            total = total[:, :width]
        mine[:, pl.ds(at.start, width)] = (inv_rms * total).astype(bf16)
        backs.append(
            [
                send(
                    mine.at[:, at],
                    gathered.at[x, z, :, at],
                    back_sems,
                    p * (outer - 1) + d - 1,
                    lax.rem(z + d, outer) * 2 + x,
                )
                for d in range(1, outer)
            ]
        )
        gathered[x, z, :, at] = mine[:, at]
    lasts = []
    for p, at in enumerate(pieces):
        for copy in backs[p]:
            copy.wait_recv()
        lasts.append(
            send(gathered.at[x, :, :, at], gathered.at[x, :, :, at], last_sems, p, partner)
        )
    for copy in lasts:
        copy.wait_recv()
    for c in range(n_kv):
        out_ref[c] = gathered[c % 2, c // 2]
    for copy in swaps + sum(sums, []) + sum(backs, []) + lasts:
        copy.wait_send()


def attend_kernel(
    heads, prior_s, accepted_s, proj_ref, parents_ref, k_ref, v_ref, cum_ref, ko_ref, vo_ref, out_ref
):
    group = k_ref.shape[0]
    length = k_ref.shape[1]
    width = heads * HEAD
    rows = group * PROPS
    score_rows = heads * PROPS
    offset = lax.axis_index("kv") * length
    step = pl.program_id(0)

    row = iota((rows, rows), 0)
    column = iota((rows, rows), 1)
    every = parents_ref[...]
    parent = jnp.concatenate(
        [
            jnp.sum(
                jnp.where(iota(every.shape, 1) == step * group + b, every, 0).astype(f32),
                axis=1,
                keepdims=True,
            ).astype(i32)
            for b in range(group)
        ],
        axis=0,
    )
    link = (parent + (row // PROPS) * PROPS == column) & (parent >= 0)
    reached = jnp.where(link | (row == column), 1.0, 0.0)
    for squaring in range((PROPS - 1).bit_length()):
        reached = jnp.minimum(
            jnp.dot(reached.astype(bf16), reached.astype(bf16), preferred_element_type=f32), 1.0
        )
    tree_gates = jnp.dot(
        reached.astype(bf16), proj_ref[:, 3 * width :], preferred_element_type=f32
    )
    lane = iota((score_rows, LANES), 1)
    row_head = iota((score_rows, LANES), 0) // PROPS
    gate_pick = jnp.where((lane % 32 == row_head) & (lane < 96), 1.0, 0.0)
    same_head = iota((score_rows, width), 0) // PROPS == iota((score_rows, width), 1) // HEAD
    position = iota((score_rows, length), 1)
    window = 2 * PROPS
    for b in range(group):
        span = slice(b * PROPS, (b + 1) * PROPS)
        seq = step * group + b
        limit = prior_s[seq] + accepted_s[seq] - offset
        owner = jnp.where((limit >= 1) & (limit <= length), 1.0, 0.0)
        new_k = proj_ref[span, width : 2 * width]
        new_v = proj_ref[span, 2 * width : 3 * width]
        query = jnp.concatenate([proj_ref[span, :width]] * heads, axis=0).astype(f32)
        query = (jnp.where(same_head, query, 0.0) * HEAD ** (-0.5)).astype(bf16)
        cum = jnp.concatenate(
            [
                jnp.broadcast_to(cum_ref[b, h : h + 1, :], (PROPS, length))
                for h in range(heads)
            ],
            axis=0,
        )
        valid = position < limit
        scores = jnp.where(valid, contract_last(query, k_ref[b]) - cum, masked_score)
        last = jnp.sum(jnp.where(position == limit - 1, cum, 0.0), axis=1, keepdims=True)
        prop_cum = last + contract_last(gate_pick, tree_gates[span], HIGHEST)
        live = jnp.concatenate([reached[span, span]] * heads, axis=0) * owner > 0.5
        tree = jnp.where(live, contract_last(query, new_k) - prop_cum, masked_score)
        top = jnp.maximum(
            jnp.max(scores, axis=1, keepdims=True), jnp.max(tree, axis=1, keepdims=True)
        )
        weights = jnp.where(valid, jnp.exp(scores - top), 0.0)
        tree_weights = jnp.where(live, jnp.exp(tree - top), 0.0)
        total = jnp.sum(weights, axis=1, keepdims=True) + jnp.sum(
            tree_weights, axis=1, keepdims=True
        )
        values = jnp.dot(weights.astype(bf16), v_ref[b], preferred_element_type=f32)
        values = values + jnp.dot(tree_weights.astype(bf16), new_v, preferred_element_type=f32)
        values = jnp.where(same_head, values, 0.0)
        t_hi, t_mid, t_low = split3(top)
        s_hi, s_mid, s_low = split3(total)
        part = lane // 16
        packed = jnp.where(
            part == 0,
            t_hi,
            jnp.where(
                part == 1, t_mid, jnp.where(part == 2, t_low, jnp.where(part == 3, s_hi, s_mid))
            ),
        )
        packed = jnp.where((lane % 16 == row_head) & (part < 5), packed, 0.0)
        picked_values = values[:PROPS]
        picked_packed = packed[:PROPS]
        for h in range(1, heads):
            picked_values = picked_values + values[h * PROPS : (h + 1) * PROPS]
            picked_packed = picked_packed + packed[h * PROPS : (h + 1) * PROPS]
        out_ref[span, :width] = picked_values.astype(bf16)
        out_ref[span, width:] = picked_packed.astype(bf16)

        start = pl.multiple_of(jnp.clip(limit, 0, length - window) // PROPS * PROPS, PROPS)
        select = start + iota((window, PROPS), 0) - limit == iota((window, PROPS), 1)
        select = jnp.where(select, 1.0, 0.0).astype(bf16)
        slot = start + iota((window, width), 0) - limit
        inside = (slot >= 0) & (slot < PROPS)
        for source, target, fresh in ((k_ref, ko_ref, new_k), (v_ref, vo_ref, new_v)):
            target[b] = source[b]
            placed = jnp.dot(select, fresh, preferred_element_type=f32)
            old = source[b, pl.ds(start, window), :].astype(f32)
            target[b, pl.ds(start, window), :] = jnp.where(inside, placed, old).astype(bf16)


def combine_kernel(
    n_kv,
    n_tp,
    heads,
    parts_ref,
    w_ref,
    out_ref,
    arrived,
    mine,
    gathered,
    partial,
    landed,
    send_a,
    recv_a,
    send_b,
    recv_b,
    send_c,
    recv_c,
):
    me = lax.axis_index("kv")
    tp = lax.axis_index("tp")
    width = heads * HEAD
    chunk_rows = parts_ref.shape[1]
    share = n_kv // n_tp
    barrier = pltpu.get_barrier_semaphore()
    for d in range(1, n_kv):
        pl.semaphore_signal(
            barrier, inc=1, device_id={"kv": lax.rem(me + d, n_kv)}, device_id_type=MESH
        )
    for d in range(1, n_tp):
        pl.semaphore_signal(
            barrier, inc=1, device_id={"tp": lax.rem(tp + d, n_tp)}, device_id_type=MESH
        )
    pl.semaphore_wait(barrier, n_kv - 1 + n_tp - 1)
    first = []
    for d in range(1, n_kv):
        peer = lax.rem(me + d, n_kv)
        copy = pltpu.make_async_remote_copy(
            src_ref=parts_ref.at[peer],
            dst_ref=arrived.at[d - 1],
            send_sem=send_a.at[d - 1],
            recv_sem=recv_a.at[d - 1],
            device_id={"kv": peer},
            device_id_type=MESH,
        )
        copy.start()
        first.append(copy)
    lane = iota((LANES, width), 0)
    fits = lane % 16 == iota((LANES, width), 1) // HEAD
    spread_top = jnp.where(fits & (lane < 48), 1.0, 0.0).astype(bf16)
    spread_sum = jnp.where(fits & (lane >= 48) & (lane < 80), 1.0, 0.0).astype(bf16)

    def unpack(block):
        packed = block[:, width:]
        return (
            jnp.dot(packed, spread_top, preferred_element_type=f32),
            jnp.dot(packed, spread_sum, preferred_element_type=f32),
            block[:, :width].astype(f32),
        )

    top, sums, values = unpack(parts_ref[me])
    for d in range(1, n_kv):
        first[d - 1].wait_recv()
        other_top, other_sums, other_values = unpack(arrived[d - 1])
        new_top = jnp.maximum(top, other_top)
        here, there = jnp.exp(top - new_top), jnp.exp(other_top - new_top)
        sums = here * sums + there * other_sums
        values = here * values + there * other_values
        top = new_top
    mine[...] = (values / sums).astype(bf16)
    second = []
    for d in range(1, n_kv):
        copy = pltpu.make_async_remote_copy(
            src_ref=mine,
            dst_ref=gathered.at[me],
            send_sem=send_b.at[d - 1],
            recv_sem=recv_b.at[d - 1],
            device_id={"kv": lax.rem(me + d, n_kv)},
            device_id_type=MESH,
        )
        copy.start()
        second.append(copy)
    gathered[me] = mine[...]
    for copy in second:
        copy.wait_recv()
    if chunk_rows % 16 == 0:
        attended = gathered[...].reshape(n_kv * chunk_rows, width)
        product = jnp.dot(attended, w_ref[...], preferred_element_type=f32).astype(bf16)
        partial[...] = product.reshape(partial.shape)
    else:

        def one(c, carry):
            partial[c] = jnp.dot(gathered[c], w_ref[...], preferred_element_type=f32).astype(bf16)
            return carry

        lax.fori_loop(0, n_kv, one, 0)
    third = []
    for d in range(1, n_tp):
        peer = lax.rem(tp + d, n_tp)
        copy = pltpu.make_async_remote_copy(
            src_ref=partial.at[pl.ds(peer * share, share)],
            dst_ref=landed.at[d - 1],
            send_sem=send_c.at[d - 1],
            recv_sem=recv_c.at[d - 1],
            device_id={"tp": peer},
            device_id_type=MESH,
        )
        copy.start()
        third.append(copy)
    total = partial[pl.ds(tp * share, share)].astype(f32)
    for d in range(1, n_tp):
        third[d - 1].wait_recv()
        total = total + landed[d - 1].astype(f32)
    out_ref[...] = total.astype(bf16)
    for copy in first + second + third:
        copy.wait_send()


def shards(
    n_kv,
    n_tp,
    tokens,
    norm_gain,
    w_query,
    w_key,
    w_value,
    w_gate,
    gate_bias,
    w_out,
    keys_cache,
    values_cache,
    cum_gates,
    prior_len,
    accepted,
    parents,
):
    row_count, depth = tokens.shape
    seq_count, length, width = keys_cache.shape
    heads = width // HEAD
    chunk_rows = row_count // n_kv
    columns = w_out.shape[1]
    vmem = pl.BlockSpec(memory_space=pltpu.VMEM)
    dma = pltpu.SemaphoreType.DMA
    proj_width = 3 * width + LANES
    out_width = width + LANES

    projected = pl.pallas_call(
        functools.partial(project_kernel, n_kv, heads),
        out_shape=jax.ShapeDtypeStruct((n_kv, chunk_rows, proj_width), bf16),
        in_specs=[vmem] * 7,
        out_specs=vmem,
        scratch_shapes=[
            pltpu.VMEM((2, n_kv // 2, chunk_rows, proj_width), bf16),
            pltpu.VMEM((n_kv // 2, chunk_rows, proj_width), bf16),
            pltpu.VMEM((n_kv // 2, chunk_rows, proj_width), bf16),
            pltpu.VMEM((n_kv // 2 - 1, chunk_rows, proj_width), bf16),
            pltpu.VMEM((2, n_kv // 2, chunk_rows, proj_width), bf16),
            pltpu.VMEM((chunk_rows, proj_width), bf16),
        ]
        + [dma((3,))] * 2
        + [dma((3 * (n_kv // 2 - 1),))] * 4
        + [dma((3,))] * 2,
        compiler_params=pltpu.CompilerParams(collective_id=0, has_side_effects=True),
        name="project",
    )(
        tokens.reshape(n_kv, chunk_rows, depth),
        norm_gain.reshape(1, depth),
        w_query,
        w_key,
        w_value,
        w_gate.T if depth % LANES == 0 else w_gate,
        gate_bias.reshape(1, -1),
    )
    projected = projected.reshape(row_count, proj_width)

    group = next(g for g in (4, 3, 2, 1) if seq_count % g == 0)
    rows = group * PROPS
    cache_spec = pl.BlockSpec((group, length, width), lambda s, *_: (s, 0, 0))
    keys_out, values_out, parts = pl.pallas_call(
        functools.partial(attend_kernel, heads),
        out_shape=(
            jax.ShapeDtypeStruct(keys_cache.shape, bf16),
            jax.ShapeDtypeStruct(values_cache.shape, bf16),
            jax.ShapeDtypeStruct((row_count, out_width), bf16),
        ),
        grid_spec=pltpu.PrefetchScalarGridSpec(
            num_scalar_prefetch=2,
            grid=(seq_count // group,),
            in_specs=[
                pl.BlockSpec((rows, proj_width), lambda s, *_: (s, 0)),
                pl.BlockSpec((PROPS, seq_count), lambda s, *_: (0, 0)),
                cache_spec,
                cache_spec,
                pl.BlockSpec((group, heads, length), lambda s, *_: (s, 0, 0)),
            ],
            out_specs=[
                cache_spec,
                cache_spec,
                pl.BlockSpec((rows, out_width), lambda s, *_: (s, 0)),
            ],
        ),
        name="attend",
    )(
        prior_len,
        accepted,
        projected,
        parents.T,
        keys_cache,
        values_cache,
        cum_gates,
    )

    mixed = pl.pallas_call(
        functools.partial(combine_kernel, n_kv, n_tp, heads),
        out_shape=jax.ShapeDtypeStruct((n_kv // n_tp, chunk_rows, columns), bf16),
        in_specs=[vmem] * 2,
        out_specs=vmem,
        scratch_shapes=[
            pltpu.VMEM((n_kv - 1, chunk_rows, out_width), bf16),
            pltpu.VMEM((chunk_rows, width), bf16),
            pltpu.VMEM((n_kv, chunk_rows, width), bf16),
            pltpu.VMEM((n_kv, chunk_rows, columns), bf16),
            pltpu.VMEM((n_tp - 1, n_kv // n_tp, chunk_rows, columns), bf16),
        ]
        + [dma((n_kv - 1,))] * 4
        + [dma((n_tp - 1,))] * 2,
        compiler_params=pltpu.CompilerParams(collective_id=1, has_side_effects=True),
        name="combine",
    )(parts.reshape(n_kv, chunk_rows, out_width), w_out)
    return (mixed.reshape(row_count // n_tp, columns), keys_out, values_out)


def solution(mesh):
    placed = (
        P(None, "kv"),
        P("kv"),
        P("kv", "tp"),
        P("kv", "tp"),
        P("kv", "tp"),
        P(),
        P(),
        P("tp", "kv"),
        P(None, "kv", "tp"),
        P(None, "kv", "tp"),
        P(None, "tp", "kv"),
        P(),
        P(),
        P(),
    )
    return jax.shard_map(
        functools.partial(shards, mesh.shape["kv"], mesh.shape["tp"]),
        mesh=mesh,
        in_specs=placed,
        out_specs=(P("tp", "kv"), P(None, "kv", "tp"), P(None, "kv", "tp")),
        check_vma=False,
    )
```
